32 devices in a mesh: sp: 8 (over z, core), tp: 4 (over y, x).
Axes of the slice: x: 2, y: 2, z: 4, core: 2. Of those that a mesh axis runs over, the one named last changes fastest.
Arguments:
- cotangent: bfloat16 [1024, 2048], P('sp'), may hold values from -6 to 6
- normed: bfloat16 [1024, 2048], P('sp'), may hold values from -6 to 6
- inverse_root_mean_square: float32 [1024], P('sp'), may hold values from 0.5 to 2
- expert_norm_scale: float32 [2048], replicated, may hold values from 0.1 to 1.9
- routes: int32 [1024, 2], P('sp'), may hold values from 0 to 7, all different within a row; in each aligned block of 128 rows (0 to 127, 128 to 255, ...) at most 64 rows name the same one
- route_probability_weight: float32 [1024, 2], P('sp'), may hold values from 0.2 to 1
- gate_weight: bfloat16 [8, 2048, 2048], P('sp', None, 'tp'), may hold values from -0.125 to 0.125
- up_weight: bfloat16 [8, 2048, 2048], P('sp', None, 'tp'), may hold values from -0.125 to 0.125
- down_weight: bfloat16 [8, 2048, 2048], P('sp', 'tp'), may hold values from -0.125 to 0.125
- recurrence_input: bfloat16 [1024, 1024], P('sp', 'tp'), may hold values from -6 to 6
- recurrence_gate_logits: bfloat16 [1024, 1024], P('sp', 'tp'), may hold values from -6 to 6
- input_gate_logits: bfloat16 [1024, 1024], P('sp', 'tp'), may hold values from -6 to 6
- channel_decay_weight: float32 [1024], P('tp'), may hold values from 3 to 20
- extra_log_decay: float32 [1024, 1024], P('sp', 'tp'), may hold values from -1 to 0
- output_matrix: bfloat16 [2048, 1024], P(None, 'tp'), may hold values from -0.1875 to 0.1875
Outputs:
- grad_gate: bfloat16 [8, 2048, 2048], P('sp', None, 'tp')
- grad_up: bfloat16 [8, 2048, 2048], P('sp', None, 'tp')
- grad_down: bfloat16 [8, 2048, 2048], P('sp', 'tp')
- grad_out_weight: float32 [2048, 1024], P('sp', 'tp')
- grad_rec_input: float32 [1024, 1024], P('sp', 'tp')
- grad_decay_gate: float32 [1024, 1024], P('sp', 'tp')
- grad_input_gate: float32 [1024, 1024], P('sp', 'tp')
The draws below stay inside these ranges and needn't reach their ends.
Inputs may be any that keep to these rules, and one draw needn't show every extreme that they name: `routes`: each row names 2 different experts; among the rows of one device no expert is named more than 64 times.
All inputs are finite; a program needn't handle non-finite values.
Results may differ from the reference program's by a relative error of at most 0.025.
Values may be sent and summed in bfloat16 or wider, within the bound.
A program may use at most 64 MiB of HBM per device.

```python
import math
import jax
import jax.numpy as jnp
import numpy as np
from jax import lax

D = 2048
C = 1024
FF = 2048
TOPK = 2
TOK_DEV = 128
EXPERTS = 8
CAP = 64
TOKENS = 1024
N_SP = 8
N_TP = 4


def draw_channel_decay_weight(key, part):
    first, second, third = jax.random.split(key, 3)
    share = 0.5
    quick = jax.random.uniform(first, (C,), jnp.float32) < share
    slow_rate = jnp.exp(jax.random.uniform(second, (C,), jnp.float32, jnp.log(0.02), jnp.log(0.12))) / TOKENS
    quick_rate = jnp.exp(jax.random.uniform(third, (C,), jnp.float32, jnp.log(0.005), jnp.log(0.02)))
    rate = jnp.where(quick, quick_rate, slow_rate)
    return (-jnp.log(jnp.expm1(rate))).astype(jnp.float32)


def draw_extra_log_decay(key, part):
    first, second = jax.random.split(key, 2)
    places = jax.random.randint(first, (3,), 0, TOKENS)
    struck = jnp.any(jnp.arange(TOKENS)[:, None] == places[None, :], axis=1)
    depth = jnp.log(jax.random.uniform(second, (TOKENS, C), jnp.float32, 0.65, 0.85))
    return jnp.where(struck[:, None], depth, 0.0).astype(jnp.float32)


def draw_recurrence_gate_logits(key, part):
    first, second = jax.random.split(key, 2)
    blocks = TOKENS // TOK_DEV
    offset = jax.random.uniform(first, (blocks,), jnp.float32, -1.0, 1.0)
    noise = jnp.clip(jax.random.normal(second, (TOKENS, C), jnp.float32) * 0.7, -3.5, 3.5)
    return (noise + jnp.repeat(offset, TOK_DEV)[:, None]).astype(jnp.bfloat16)


def raised(drawn, own_key, source, target, shards_of, factor):
    owner, partner = [(jnp.arange(drawn.shape[position]) // (drawn.shape[position] // shards_of)).reshape([-1 if axis == position else 1 for axis in range(drawn.ndim)]) for position in (source, target)]
    chosen = jax.random.permutation(own_key, shards_of)[partner]
    strong = (owner == chosen) | (owner == (partner + shards_of // 2) % shards_of)
    return jnp.where(strong, factor * drawn, drawn)


def shard_levels(stream_key, extent, cuts, least, largest):
    factor_of, own = 1.0, jax.random.fold_in(stream_key, 6)
    for axis_at, parts in cuts:
        draws = jnp.exp(jax.random.uniform(jax.random.fold_in(own, axis_at), (parts,), jnp.float32, least / len(cuts), largest / len(cuts)))
        factor_of = factor_of * jnp.repeat(draws, extent[axis_at] // parts).reshape([-1 if axis == axis_at else 1 for axis in range(len(extent))])
    return factor_of


def routed_block(key, own, number, rows, number_of, top, most, lean):
    order = jax.random.permutation(key, number_of)
    packed, ordinary = shares(number_of, rows * top, most, lean, True), shares(number_of, rows * top, most, lean, False)
    places = jnp.arange(number_of)

    def named(tallies, rotation):
        used = int((tallies > 0).sum())
        fixed = max(1, used // 4)
        moved = fixed + (places - fixed + rotation * (used - fixed)) % max(1, number_of - fixed)
        return jnp.zeros((number_of,), jnp.int32).at[order[jnp.where(places < fixed, places, moved)]].set(jnp.asarray(tallies, jnp.int32))

    tallies = jnp.where(number % 4 == 0, named(packed, number // 4), named(ordinary, number - number // 4 - 1))
    mixed = jax.random.permutation(jax.random.fold_in(own, 3), number_of)
    source_of, receiver = mixed[0:number_of // 2 * 2:2], mixed[1:number_of // 2 * 2:2]
    room = jnp.minimum(tallies[source_of] - 1, most - tallies[receiver]) // 2
    room = jnp.where((source_of == order[0]) | (receiver == order[0]) | (tallies[receiver] == 0), 0, jnp.maximum(room, 0))
    moved = jax.random.randint(jax.random.fold_in(own, 4), (number_of // 2,), 0, 1 << 20) % (room + 1)
    tallies = tallies.at[source_of].add(-moved).at[receiver].add(moved)
    items = jnp.searchsorted(jnp.cumsum(tallies), jnp.arange(rows * top), side="right").astype(jnp.int32)
    listing = items.reshape(top, rows).T
    listing = listing[jax.random.permutation(jax.random.fold_in(own, 1), rows)]
    rotation = jax.random.randint(jax.random.fold_in(own, 2), (rows, 1), 0, top)
    return jnp.take_along_axis(listing, (jnp.arange(top)[None, :] + rotation) % top, axis=1)


def shares(amount, total, most, lean, full):
    loads = [(1 << 20) // math.isqrt(grade ** lean) + 1 for grade in range(1, amount + 1)]
    largest = most if full else min(most, max(-(-total // amount), total * loads[0] // sum(loads)))
    least = 1 if total - largest >= amount - 1 else 0
    holding, rest = [largest] + [least] * (amount - 1), total - largest - least * (amount - 1)
    while rest > 0:
        candidates = [i for i in range(1, amount) if holding[i] < largest] or [i for i in range(1, amount) if holding[i] < most]
        pool, remaining = sum([loads[i] for i in candidates]), rest
        for i in candidates:
            addition = min(most - holding[i], max(1, remaining * loads[i] // pool), rest)
            holding[i] = holding[i] + addition
            rest = rest - addition
    return np.array(holding)


def gaussian(rng, shape, width, reach, cuts=(), kind=jnp.bfloat16):
    loudness = shard_levels(rng, shape, cuts, -0.22, 0.18) if cuts else 1.0
    values = jax.random.normal(rng, shape, jnp.float32) * width * loudness
    return jnp.minimum(jnp.maximum(values, -reach), reach).astype(kind)


def gaussian_with(own_key, extent, scale, bound, shards, heavy, kind=jnp.bfloat16):
    entries = scale * jax.random.normal(own_key, extent, jnp.float32)
    if shards:
        entries = entries * shard_levels(own_key, extent, shards, -0.22, 0.18)
    return jnp.clip(raised(entries, jax.random.fold_in(own_key, 3), *heavy), -bound, bound).astype(kind)


def setup_inputs(seed: int = 0) -> dict:
    key_list = jax.random.split(jax.random.key(seed), 16)
    cotangent = gaussian_with(key_list[0], (TOKENS, D), 1.0, 6.0, ((0, 8),), (0, 1, 8, 2.0))
    normed = gaussian(key_list[1], (TOKENS, D), 1.0, 6.0, ((0, 8),))
    inverse_root_mean_square = jnp.clip(jnp.exp(math.log(2.0) - 1.3862944 * jax.random.uniform(key_list[2], (TOKENS,), jnp.float32) ** shard_levels(key_list[2], (TOKENS,), ((0, 8),), -0.2, 0.2)), 0.5, 2.0)
    expert_norm_scale = jnp.clip(1.0 + 0.18 * jax.random.normal(key_list[3], (D,), jnp.float32), 0.1, 1.9)
    routes_keys = jax.random.split(jax.random.fold_in(key_list[4], 1), TOKENS // TOK_DEV)
    routes_turns = jax.random.permutation(jax.random.fold_in(key_list[4], 3), TOKENS // TOK_DEV)
    routes = jax.vmap(lambda own, number: routed_block(jax.random.fold_in(key_list[4], 2), own, number, TOK_DEV, EXPERTS, TOPK, CAP, 1))(routes_keys, routes_turns).reshape((TOKENS, TOPK))
    route_probability_weight = jnp.clip(0.2 + 0.8 * jax.random.uniform(key_list[5], (TOKENS, TOPK), jnp.float32) ** shard_levels(key_list[5], (TOKENS, TOPK), ((0, 8),), -0.2, 0.2), 0.2, 1.0)
    gate_weight = gaussian(key_list[6], (EXPERTS, D, FF), D ** -0.5, 0.125, ((0, 8), (2, 4)))
    up_weight = gaussian(key_list[7], (EXPERTS, D, FF), D ** -0.5, 0.125, ((0, 8), (2, 4)))
    down_weight = gaussian(key_list[8], (EXPERTS, FF, D), FF ** -0.5, 0.125, ((0, 8), (1, 4)))
    recurrence_input = gaussian(key_list[9], (TOKENS, C), 1.0, 6.0, ((0, 8), (1, 4)))
    recurrence_gate_logits = draw_recurrence_gate_logits(jax.random.fold_in(key_list[15], 71), 0)
    input_gate_logits = gaussian(key_list[11], (TOKENS, C), 1.0, 6.0, ((0, 8), (1, 4)))
    channel_decay_weight = draw_channel_decay_weight(jax.random.fold_in(key_list[15], 71), 0)
    extra_log_decay = draw_extra_log_decay(jax.random.fold_in(key_list[15], 71), 0)
    output_matrix = gaussian(key_list[14], (D, C), C ** -0.5, 0.1875, ((1, 4),))
    return dict(cotangent=cotangent, normed=normed, inverse_root_mean_square=inverse_root_mean_square, expert_norm_scale=expert_norm_scale, routes=routes, route_probability_weight=route_probability_weight, gate_weight=gate_weight, up_weight=up_weight, down_weight=down_weight, recurrence_input=recurrence_input, recurrence_gate_logits=recurrence_gate_logits, input_gate_logits=input_gate_logits, channel_decay_weight=channel_decay_weight, extra_log_decay=extra_log_decay, output_matrix=output_matrix)


def link(earlier, later):
    return (earlier[0] * later[0], later[0] * earlier[1] + later[1])

def expert_step(items):
    grad_in, tokens_in, gate_w, up_w, down_w = items
    rows = tokens_in.shape[0]
    gate_pre = jnp.dot(tokens_in, gate_w, preferred_element_type=jnp.float32)
    up_pre = jnp.dot(tokens_in, up_w, preferred_element_type=jnp.float32)
    sigma = jax.nn.sigmoid(gate_pre)
    swish = gate_pre * sigma
    active = (swish * up_pre).astype(jnp.bfloat16)
    d_active = jnp.dot(grad_in, down_w.T, preferred_element_type=jnp.float32)
    d_gate = (d_active * up_pre * sigma * (1.0 + gate_pre * (1.0 - sigma))).astype(jnp.bfloat16)
    d_up = (d_active * swish).astype(jnp.bfloat16)
    grad_down = jnp.dot(active.T, grad_in, preferred_element_type=jnp.float32).astype(jnp.bfloat16)
    grad_gate = jnp.dot(tokens_in.T, d_gate, preferred_element_type=jnp.float32).astype(jnp.bfloat16)
    grad_up = jnp.dot(tokens_in.T, d_up, preferred_element_type=jnp.float32).astype(jnp.bfloat16)
    block = FF // N_TP
    d_gate4 = d_gate.astype(jnp.float32).reshape(rows, N_TP, block)
    d_up4 = d_up.astype(jnp.float32).reshape(rows, N_TP, block)
    gate4 = gate_w.astype(jnp.float32).reshape(D, N_TP, block)
    up4 = up_w.astype(jnp.float32).reshape(D, N_TP, block)
    pieces = jnp.einsum('rjf,djf->jrd', d_gate4, gate4) + jnp.einsum('rjf,djf->jrd', d_up4, up4)
    rounded = lax.optimization_barrier(pieces.astype(jnp.bfloat16)).astype(jnp.float32)
    returned = lax.optimization_barrier(jnp.sum(rounded, axis=0)).astype(jnp.bfloat16)
    return (grad_gate, grad_up, grad_down, returned)

def reference(cotangent, normed, inverse_root_mean_square, expert_norm_scale, routes, route_probability_weight, gate_weight, up_weight, down_weight, recurrence_input, recurrence_gate_logits, input_gate_logits, channel_decay_weight, extra_log_decay, output_matrix):
    per_block = TOK_DEV * TOPK
    chosen = routes.reshape(N_SP, per_block)
    member = (chosen[:, :, None] == jnp.arange(EXPERTS, dtype=jnp.int32)[None, None, :]).astype(jnp.int32)
    ranking = lax.optimization_barrier(jnp.sum((jnp.cumsum(member, axis=1) - member) * member, axis=2))
    source = jnp.arange(N_SP, dtype=jnp.int32)[:, None]
    landing = (chosen * (N_SP * CAP) + source * CAP + ranking).reshape(-1).astype(jnp.int32)
    scaled = (route_probability_weight[:, :, None] * cotangent[:, None, :].astype(jnp.float32)).astype(jnp.bfloat16)
    scaled = scaled.reshape(TOKENS * TOPK, D)
    copies = jnp.repeat(normed, TOPK, axis=0)
    buffer_rows = EXPERTS * N_SP * CAP
    grad_in = jnp.zeros((buffer_rows, D), jnp.bfloat16).at[landing].set(scaled).reshape(EXPERTS, N_SP * CAP, D)
    tokens_in = jnp.zeros((buffer_rows, D), jnp.bfloat16).at[landing].set(copies).reshape(EXPERTS, N_SP * CAP, D)
    grad_gate, grad_up, grad_down, returned = lax.map(expert_step, (grad_in, tokens_in, gate_weight, up_weight, down_weight))
    back_rows = returned.reshape(buffer_rows, D)[landing]
    d_norm = lax.optimization_barrier(jnp.sum(back_rows.astype(jnp.float32).reshape(TOKENS, TOPK, D), axis=1))
    nhat = normed.astype(jnp.float32) / expert_norm_scale[None, :]
    gained = expert_norm_scale[None, :] * d_norm
    stat = lax.optimization_barrier(jnp.mean(gained * nhat, axis=1, keepdims=True))
    d_mix = (cotangent.astype(jnp.float32) + inverse_root_mean_square[:, None] * (gained - nhat * stat)).astype(jnp.bfloat16)
    retention_factor = jax.nn.sigmoid(recurrence_gate_logits.astype(jnp.float32))
    admit = jax.nn.sigmoid(input_gate_logits.astype(jnp.float32))
    signal = recurrence_input.astype(jnp.float32)
    decay_speed = jax.nn.softplus(-channel_decay_weight)
    log_retention = -8.0 * retention_factor * decay_speed[None, :] + extra_log_decay
    keep = jnp.exp(log_retention)
    scale_in = jnp.sqrt(-jnp.expm1(2.0 * log_retention))
    driven = scale_in * admit * signal
    _, state = lax.associative_scan(link, (keep, driven), axis=0)
    hidden = state.astype(jnp.bfloat16)
    state_prev = jnp.concatenate([jnp.zeros((1, C), jnp.float32), state[:-1]], axis=0)
    grad_out_weight = jnp.dot(d_mix.T, hidden, preferred_element_type=jnp.float32)
    d_state = jnp.dot(d_mix, output_matrix, preferred_element_type=jnp.float32)
    keep_next = jnp.concatenate([keep[1:], jnp.ones((1, C), jnp.float32)], axis=0)
    _, total = lax.associative_scan(link, (keep_next, d_state), reverse=True, axis=0)
    grad_rec_input = total * scale_in * admit
    grad_input_gate = total * scale_in * signal * admit * (1.0 - admit)
    d_log = total * state_prev * keep - total * admit * signal * keep * keep / scale_in
    grad_decay_gate = d_log * (-8.0 * decay_speed[None, :]) * retention_factor * (1.0 - retention_factor)
    return (grad_gate, grad_up, grad_down, grad_out_weight, grad_rec_input, grad_decay_gate, grad_input_gate)
```

```python
import functools

import jax
import jax.numpy as jnp
from jax import lax
from jax.experimental import pallas as pl
from jax.experimental.pallas import tpu as pltpu
from jax.sharding import PartitionSpec as P

MESH = pl.DeviceIdType.MESH
VMEM_LIMIT = 56 * 1024 * 1024


def greet(n, m, me, j):
    barrier = pltpu.get_barrier_semaphore()
    for k in range(1, n):
        pl.semaphore_signal(
            barrier, inc=1, device_id={"sp": lax.rem(me + k, n)}, device_id_type=MESH
        )
    for p in range(1, m):
        pl.semaphore_signal(
            barrier, inc=1, device_id={"tp": lax.rem(j + p, m)}, device_id_type=MESH
        )
    pl.semaphore_wait(barrier, n - 1 + m - 1)


def send(src, dst, send_sem, recv_sem, where):
    return pltpu.make_async_remote_copy(
        src_ref=src,
        dst_ref=dst,
        send_sem=send_sem,
        recv_sem=recv_sem,
        device_id=where,
        device_id_type=MESH,
    )


def scan_rows(a, b, reverse):
    rows = a.shape[0]
    place = lax.broadcasted_iota(jnp.int32, a.shape, 0)
    step = 1
    while step < rows:
        if reverse:
            known = place < rows - step
            shift = rows - step
        else:
            known = place >= step
            shift = step
        a_far = jnp.where(known, pltpu.roll(a, shift, 0), 1.0)
        b_far = jnp.where(known, pltpu.roll(b, shift, 0), 0.0)
        b = a * b_far + b
        a = a * a_far
        step *= 2
    return a, b


def dispatch_kernel(
    n, m, xs, ys, keep, driven, xo, yo, hidden, prev, carry,
    cum, loc, s1s, s1r, s2s, s2r, cs, cr, lsem,
):
    me, j = lax.axis_index("sp"), lax.axis_index("tp")
    cap, q = xs.shape[0] // n, xs.shape[1]
    tok = keep.shape[0]
    rows = lambda s: pl.ds(pl.multiple_of(s * cap, cap), cap)
    cols = lambda t: pl.ds(pl.multiple_of(t * q, q), q)
    pairs = ((0, xs, xo), (1, ys, yo))
    a, b = scan_rows(keep[...], driven[...], False)
    cum[...] = a
    loc[...] = b
    width = a.shape[1]
    carry[me] = jnp.concatenate(
        [a[tok - 1 : tok], b[tok - 1 : tok], jnp.zeros((6, width), jnp.float32)], axis=0
    )
    greet(n, m, me, j)

    def first(k):
        to = lax.rem(me + k, n)
        return [
            send(s.at[rows(to)], o.at[rows(me), cols(j)], s1s.at[i], s1r.at[i, k], {"sp": to})
            for i, s, o in pairs
        ]

    def carried(k):
        to = lax.rem(me + k, n)
        return send(carry.at[me], carry.at[me], cs.at[k], cr.at[k], {"sp": to})

    own = [
        pltpu.make_async_copy(s.at[rows(me)], o.at[rows(me), cols(j)], lsem.at[i])
        for i, s, o in pairs
    ]
    for c in own:
        c.start()

    def start_carry(k, _):
        carried(k).start()
        return 0

    lax.fori_loop(1, n, start_carry, 0)

    def start_first(k, _):
        for c in first(k):
            c.start()
        return 0

    lax.fori_loop(1, n, start_first, 0)

    def forward(source):
        for p in range(1, m):
            for i, _, o in pairs:
                block = o.at[rows(source), cols(j)]
                send(block, block, s2s.at[i, p], s2r.at[i, p], {"tp": lax.rem(j + p, m)}).start()

    for c in own:
        c.wait()
    forward(me)

    def relay(k, _):
        source = lax.rem(me - k + n, n)
        for i, s, o in pairs:
            block = o.at[rows(source), cols(j)]
            send(block, block, s1s.at[i], s1r.at[i, k], {"sp": source}).wait_recv()
        forward(source)
        return 0

    lax.fori_loop(1, n, relay, 0)

    def take_carry(k, _):
        source = lax.rem(me - k + n, n)
        send(carry.at[source], carry.at[source], cs.at[k], cr.at[k], {"sp": source}).wait_recv()
        carried(k).wait_send()
        return 0

    lax.fori_loop(1, n, take_carry, 0)
    state = jnp.zeros((1, width), jnp.float32)
    for s in range(n):
        state = jnp.where(s < me, carry[s, 0:1] * state + carry[s, 1:2], state)
    whole = loc[...] + cum[...] * state
    hidden[...] = whole.astype(hidden.dtype)
    place = lax.broadcasted_iota(jnp.int32, whole.shape, 0)
    prev[...] = jnp.where(place >= 1, pltpu.roll(whole, 1, 0), state)
    for i, s, o in pairs:
        part = s.at[pl.ds(0, (n - 1) * cap)]
        send(part, part, s1s.at[i], s1r.at[i, 0], {"sp": lax.rem(me + 1, n)}).wait_send()
        for p in range(1, m):
            far = lax.rem(j - p + m, m)
            mine, theirs = o.at[:, cols(j)], o.at[:, cols(far)]
            send(mine, mine, s2s.at[i, p], s2r.at[i, p], {"tp": far}).wait_send()
            send(theirs, theirs, s2s.at[i, p], s2r.at[i, p], {"tp": far}).wait_recv()


def return_kernel(
    n, m, pr, pick, hid, out, hid_all,
    stage, red, back, rs, rr, bs, br, gs, gr, hs, hr, lsem,
):
    me, j = lax.axis_index("sp"), lax.axis_index("tp")
    tok = hid.shape[0]
    cap, q = pr.shape[0] // n, pr.shape[1] // m
    rows = lambda s: pl.ds(pl.multiple_of(s * cap, cap), cap)
    cols = lambda t: pl.ds(pl.multiple_of(t * q, q), q)
    greet(n, m, me, j)
    own = pltpu.make_async_copy(hid, hid_all.at[me], lsem)
    own.start()

    def spread(k, _):
        to = lax.rem(me + k, n)
        for p in range(1, m):
            far = lax.rem(j + p, m)
            send(
                pr.at[rows(to), cols(far)],
                stage.at[p - 1, rows(to)],
                rs.at[k],
                rr.at[k],
                {"tp": far},
            ).start()
        return 0

    lax.fori_loop(1, n + 1, spread, 0)

    def share(k, _):
        to = lax.rem(me + k, n)
        send(hid, hid_all.at[me], hs.at[k], hr.at[k], {"sp": to}).start()
        return 0

    lax.fori_loop(1, n, share, 0)

    def ship(k):
        to = lax.rem(me + k, n)
        return send(red.at[rows(to)], back.at[rows(me)], bs.at[k], br.at[k], {"sp": to})

    def reduce(k, _):
        to = lax.rem(me + k, n)
        block = stage.at[:, rows(to)]
        got = send(block, block, rs.at[k], rr.at[k], {"tp": lax.rem(j + 1, m)})
        got.wait_recv()
        got.wait_send()
        total = pr[rows(to), cols(j)].astype(jnp.float32)
        for p in range(1, m):
            total = total + stage[p - 1, rows(to)].astype(jnp.float32)
        red[rows(to)] = total.astype(red.dtype)

        @pl.when(k > 1)
        def _():
            ship(k - 1).start()

        return 0

    lax.fori_loop(1, n + 1, reduce, 0)
    back[rows(me)] = red[rows(me)]

    def collect(k, _):
        source = lax.rem(me - k + n, n)
        block = back.at[rows(source)]
        send(block, block, bs.at[k], br.at[k], {"sp": source}).wait_recv()
        return 0

    lax.fori_loop(1, n, collect, 0)
    total = jnp.dot(pick[...], back[...], preferred_element_type=jnp.float32)
    out[:, cols(j)] = total.astype(out.dtype)

    def finish(k, _):
        source = lax.rem(me - k + n, n)
        ship(k).wait_send()
        got = send(hid, hid_all.at[source], hs.at[k], hr.at[k], {"sp": source})
        got.wait_recv()
        got.wait_send()
        return 0

    lax.fori_loop(1, n, finish, 0)
    own.wait()
    mine = out.at[:, cols(j)]
    for p in range(1, m):
        send(mine, mine, gs.at[p], gr.at[p], {"tp": lax.rem(j + p, m)}).start()
    for p in range(1, m):
        far = lax.rem(j - p + m, m)
        theirs = out.at[:, cols(far)]
        send(mine, mine, gs.at[p], gr.at[p], {"tp": far}).wait_send()
        send(theirs, theirs, gs.at[p], gr.at[p], {"tp": far}).wait_recv()


def last_kernel(
    n, m, mix_t, hid_all, d_state, keep, carry, total, gow,
    got, cum, loc, back, ms, mr, cs, cr, lsem,
):
    me, j = lax.axis_index("sp"), lax.axis_index("tp")
    tok, width = keep.shape
    slab = mix_t.shape[0] // n
    rows = lambda s: pl.ds(pl.multiple_of(s * slab, slab), slab)
    greet(n, m, me, j)
    own = pltpu.make_async_copy(mix_t.at[rows(me)], got.at[me], lsem)
    own.start()

    def blocks(k):
        to = lax.rem(me + k, n)
        return send(mix_t.at[rows(to)], got.at[me], ms.at[k], mr.at[k], {"sp": to})

    def carried(k):
        to = lax.rem(me + k, n)
        return send(back.at[me], back.at[me], cs.at[k], cr.at[k], {"sp": to})

    place = lax.broadcasted_iota(jnp.int32, (tok, width), 0)
    here = keep[...]
    after = jnp.where(place < tok - 1, pltpu.roll(here, tok - 1, 0), 1.0)
    a, b = scan_rows(after, d_state[...], True)
    cum[...] = a
    loc[...] = b
    back[me] = jnp.broadcast_to(here[0:1] * b[0:1], (8, width))
    own.wait()

    def start(k, _):
        carried(k).start()
        return 0

    lax.fori_loop(1, n, start, 0)

    def start_blocks(k, _):
        blocks(k).start()
        return 0

    lax.fori_loop(1, n, start_blocks, 0)

    def take(k, _):
        source = lax.rem(me - k + n, n)
        send(back.at[source], back.at[source], cs.at[k], cr.at[k], {"sp": source}).wait_recv()
        carried(k).wait_send()
        return 0

    lax.fori_loop(1, n, take, 0)
    enter = jnp.zeros((1, width), jnp.float32)
    for s in range(n - 1, -1, -1):
        enter = jnp.where(s > me, carry[s, 0:1] * enter + back[s, 0:1], enter)
    total[...] = loc[...] + cum[...] * enter
    gow[...] = jnp.dot(got[me], hid_all[me], preferred_element_type=jnp.float32)

    def add(k, _):
        source = lax.rem(me - k + n, n)
        send(got.at[source], got.at[source], ms.at[k], mr.at[k], {"sp": source}).wait_recv()
        blocks(k).wait_send()
        gow[...] += jnp.dot(got[source], hid_all[source], preferred_element_type=jnp.float32)
        return 0

    lax.fori_loop(1, n, add, 0)


def call(kernel, n, m, outs, scratch, ident, *args):
    return pl.pallas_call(
        functools.partial(kernel, n, m),
        out_shape=tuple(jax.ShapeDtypeStruct(s, d) for s, d in outs),
        in_specs=[pl.BlockSpec(memory_space=pltpu.VMEM)] * len(args),
        out_specs=tuple(pl.BlockSpec(memory_space=pltpu.VMEM) for _ in outs),
        scratch_shapes=scratch,
        compiler_params=pltpu.CompilerParams(
            collective_id=ident, has_side_effects=True, vmem_limit_bytes=VMEM_LIMIT
        ),
    )(*args)


def shards(
    cotangent,
    normed,
    inverse_root_mean_square,
    expert_norm_scale,
    routes,
    route_probability_weight,
    gate_weight,
    up_weight,
    down_weight,
    recurrence_input,
    recurrence_gate_logits,
    input_gate_logits,
    channel_decay_weight,
    extra_log_decay,
    output_matrix,
):
    tok_rows, features = normed.shape
    n, m = lax.axis_size("sp"), lax.axis_size("tp")
    picks = routes.shape[1]
    capacity = 2 * picks * tok_rows // n
    slots = n * capacity
    q = features // m
    channels = recurrence_input.shape[1]
    f32, bf16 = jnp.float32, jnp.bfloat16
    dma = pltpu.SemaphoreType.DMA
    rowdims = (((0,), (0,)), ((), ()))
    coldims = (((1,), (1,)), ((), ()))

    chosen = routes.reshape(-1)
    member = chosen[:, None] == jnp.arange(n, dtype=jnp.int32)[None, :]
    order = jnp.arange(chosen.shape[0])
    below = (order[:, None] > order[None, :]).astype(bf16)
    before = jnp.dot(below, member.astype(bf16), preferred_element_type=f32)
    ranking = jnp.sum(jnp.where(member, before, 0.0), axis=1).astype(jnp.int32)
    landing = (chosen * capacity + ranking).reshape(tok_rows, picks)
    slot = jnp.arange(slots, dtype=jnp.int32)
    hits = [slot[:, None] == landing[:, k][None, :] for k in range(picks)]
    place = functools.reduce(jnp.logical_or, hits).astype(bf16)
    pick = functools.reduce(
        jnp.logical_or, [landing[:, k][:, None] == slot[None, :] for k in range(picks)]
    ).astype(bf16)
    share = sum(
        jnp.sum(jnp.where(h, route_probability_weight[:, k][None, :], 0.0), axis=1)
        for k, h in enumerate(hits)
    )
    offset = lax.axis_index("tp") * q
    normed_part = lax.dynamic_slice_in_dim(normed, offset, q, 1)
    cot_part = lax.dynamic_slice_in_dim(cotangent, offset, q, 1)
    token_send = jnp.dot(place, normed_part, preferred_element_type=f32).astype(bf16)
    grad_send = (
        share[:, None] * jnp.dot(place, cot_part, preferred_element_type=f32)
    ).astype(bf16)

    retention_factor = jax.nn.sigmoid(recurrence_gate_logits.astype(f32))
    admit = jax.nn.sigmoid(input_gate_logits.astype(f32))
    signal = recurrence_input.astype(f32)
    decay_speed = jax.nn.softplus(-channel_decay_weight)
    log_retention = -8.0 * retention_factor * decay_speed[None, :] + extra_log_decay
    keep = jnp.exp(log_retention)
    scale_in = jnp.sqrt(-jnp.expm1(2.0 * log_retention))
    driven = scale_in * admit * signal

    token_recv, grad_recv, hidden, state_prev, carry = call(
        dispatch_kernel, n, m,
        [
            ((slots, features), bf16),
            ((slots, features), bf16),
            ((tok_rows, channels), bf16),
            ((tok_rows, channels), f32),
            ((n, 8, channels), f32),
        ],
        [
            pltpu.VMEM((tok_rows, channels), f32),
            pltpu.VMEM((tok_rows, channels), f32),
            dma((2,)),
            dma((2, n)),
            dma((2, m)),
            dma((2, m)),
            dma((n,)),
            dma((n,)),
            dma((2,)),
        ],
        0, token_send, grad_send, keep, driven,
    )

    gate_w = gate_weight[0]
    up_w = up_weight[0]
    down_w = down_weight[0]
    gate_pre = jnp.dot(token_recv, gate_w, preferred_element_type=f32)
    up_pre = jnp.dot(token_recv, up_w, preferred_element_type=f32)
    sigma = jax.nn.sigmoid(gate_pre)
    swish = gate_pre * sigma
    active = (swish * up_pre).astype(bf16)
    d_active = lax.dot_general(grad_recv, down_w, coldims, preferred_element_type=f32)
    d_gate = (d_active * up_pre * sigma * (1.0 + gate_pre * (1.0 - sigma))).astype(bf16)
    d_up = (d_active * swish).astype(bf16)
    grad_down = lax.dot_general(active, grad_recv, rowdims, preferred_element_type=f32).astype(bf16)
    grad_gate = lax.dot_general(token_recv, d_gate, rowdims, preferred_element_type=f32).astype(bf16)
    grad_up = lax.dot_general(token_recv, d_up, rowdims, preferred_element_type=f32).astype(bf16)
    partial_rows = lax.dot_general(d_gate, gate_w, coldims, preferred_element_type=f32)
    partial_rows = partial_rows + lax.dot_general(d_up, up_w, coldims, preferred_element_type=f32)

    d_norm, hidden_all = call(
        return_kernel, n, m,
        [((tok_rows, features), bf16), ((n, tok_rows, channels), bf16)],
        [
            pltpu.VMEM((m - 1, slots, q), bf16),
            pltpu.VMEM((slots, q), bf16),
            pltpu.VMEM((slots, q), bf16),
            dma((n + 1,)),
            dma((n + 1,)),
            dma((n,)),
            dma((n,)),
            dma((m,)),
            dma((m,)),
            dma((n,)),
            dma((n,)),
            dma,
        ],
        1, partial_rows.astype(bf16), pick, hidden,
    )
    d_norm = d_norm.astype(f32)
    nhat = normed.astype(f32) / expert_norm_scale[None, :]
    gained = expert_norm_scale[None, :] * d_norm
    stat = jnp.mean(gained * nhat, axis=1, keepdims=True)
    d_mix = (
        cotangent.astype(f32) + inverse_root_mean_square[:, None] * (gained - nhat * stat)
    ).astype(bf16)
    d_state = jnp.dot(d_mix, output_matrix, preferred_element_type=f32)

    total, grad_out_weight = call(
        last_kernel, n, m,
        [((tok_rows, channels), f32), ((features // n, channels), f32)],
        [
            pltpu.VMEM((n, features // n, tok_rows), bf16),
            pltpu.VMEM((tok_rows, channels), f32),
            pltpu.VMEM((tok_rows, channels), f32),
            pltpu.VMEM((n, 8, channels), f32),
            dma((n,)),
            dma((n,)),
            dma((n,)),
            dma((n,)),
            dma,
        ],
        2, d_mix.T, hidden_all, d_state, keep, carry,
    )
    grad_rec_input = total * scale_in * admit
    grad_input_gate = total * scale_in * signal * admit * (1.0 - admit)
    d_log = total * state_prev * keep - total * admit * signal * keep * keep / scale_in
    grad_decay_gate = (
        d_log * (-8.0 * decay_speed[None, :]) * retention_factor * (1.0 - retention_factor)
    )
    return (
        grad_gate[None],
        grad_up[None],
        grad_down[None],
        grad_out_weight,
        grad_rec_input,
        grad_decay_gate,
        grad_input_gate,
    )


def solution(mesh):
    return jax.shard_map(
        shards,
        mesh=mesh,
        in_specs=(
            P("sp", None),
            P("sp", None),
            P("sp"),
            P(),
            P("sp", None),
            P("sp", None),
            P("sp", None, "tp"),
            P("sp", None, "tp"),
            P("sp", "tp", None),
            P("sp", "tp"),
            P("sp", "tp"),
            P("sp", "tp"),
            P("tp"),
            P("sp", "tp"),
            P(None, "tp"),
        ),
        out_specs=(
            P("sp", None, "tp"),
            P("sp", None, "tp"),
            P("sp", "tp", None),
            P("sp", "tp"),
            P("sp", "tp"),
            P("sp", "tp"),
            P("sp", "tp"),
        ),
        check_vma=False,
    )
```

```python
import functools

import jax
import jax.numpy as jnp
from jax import lax
from jax.experimental import pallas as pl
from jax.experimental.pallas import tpu as pltpu
from jax.sharding import PartitionSpec as P

MESH = pl.DeviceIdType.MESH
VMEM_LIMIT = 56 * 1024 * 1024


def sides(m):
    high = max(d for d in range(1, m + 1) if m % d == 0 and d * d <= m)
    return high, m // high


def greet(n, m, me, j):
    barrier = pltpu.get_barrier_semaphore()
    for k in range(1, n):
        pl.semaphore_signal(
            barrier, inc=1, device_id={"sp": lax.rem(me + k, n)}, device_id_type=MESH
        )
    for p in range(1, m):
        pl.semaphore_signal(
            barrier, inc=1, device_id={"tp": lax.rem(j + p, m)}, device_id_type=MESH
        )
    pl.semaphore_wait(barrier, n - 1 + m - 1)


def send(src, dst, send_sem, recv_sem, where):
    return pltpu.make_async_remote_copy(
        src_ref=src,
        dst_ref=dst,
        send_sem=send_sem,
        recv_sem=recv_sem,
        device_id=where,
        device_id_type=MESH,
    )


def scan_rows(a, b, reverse):
    rows = a.shape[0]
    place = lax.broadcasted_iota(jnp.int32, a.shape, 0)
    step = 1
    while step < rows:
        if reverse:
            known = place < rows - step
            shift = rows - step
        else:
            known = place >= step
            shift = step
        a_far = jnp.where(known, pltpu.roll(a, shift, 0), 1.0)
        b_far = jnp.where(known, pltpu.roll(b, shift, 0), 0.0)
        b = a * b_far + b
        a = a * a_far
        step *= 2
    return a, b


def dispatch_kernel(
    n, m, xs, ys, keep, driven, xo, yo, hidden, prev, carry,
    cum, loc, s1s, s1r, f1s, f1r, f2s, f2r, cs, cr, lsem,
):
    me, j = lax.axis_index("sp"), lax.axis_index("tp")
    cap, q = xs.shape[0] // n, xs.shape[1]
    tok = keep.shape[0]
    rows = lambda s: pl.ds(pl.multiple_of(s * cap, cap), cap)
    cols = lambda t: pl.ds(pl.multiple_of(t * q, q), q)
    pairs = ((0, xs, xo), (1, ys, yo))
    high, low = sides(m)
    upper, lower = lax.div(j, low), lax.rem(j, low)

    def size(i):
        return low if i == 0 else high

    def near(i, along, across):
        up, down = (across, along) if i == 0 else (along, across)
        return lax.rem(upper + up, high) * low + lax.rem(lower + down, low)

    a, b = scan_rows(keep[...], driven[...], False)
    cum[...] = a
    loc[...] = b
    width = a.shape[1]
    carry[me] = jnp.concatenate(
        [a[tok - 1 : tok], b[tok - 1 : tok], jnp.zeros((6, width), jnp.float32)], axis=0
    )
    greet(n, m, me, j)

    def first(k):
        to = lax.rem(me + k, n)
        return [
            send(s.at[rows(to)], o.at[rows(me), cols(j)], s1s.at[i], s1r.at[i, k], {"sp": to})
            for i, s, o in pairs
        ]

    def carried(k):
        to = lax.rem(me + k, n)
        return send(carry.at[me], carry.at[me], cs.at[k], cr.at[k], {"sp": to})

    own = [
        pltpu.make_async_copy(s.at[rows(me)], o.at[rows(me), cols(j)], lsem.at[i])
        for i, s, o in pairs
    ]
    for c in own:
        c.start()

    def start_carry(k, _):
        carried(k).start()
        return 0

    lax.fori_loop(1, n, start_carry, 0)

    def start_first(k, _):
        for c in first(k):
            c.start()
        return 0

    lax.fori_loop(1, n, start_first, 0)

    def onward(k, i, o):
        source = lax.rem(me - k + n, n)
        block = o.at[rows(source), cols(j)]
        for p in range(1, size(i)):
            send(block, block, f1s.at[i, p], f1r.at[i, p, k], {"tp": near(i, p, 0)}).start()
        for p in range(1, size(1 - i)):
            send(block, block, f2s.at[i, p, 0], f2r.at[i, p, 0], {"tp": near(i, 0, p)}).start()

    def relayed(k, i, o):
        source = lax.rem(me - k + n, n)
        for c in range(1, size(i)):
            far = near(i, size(i) - c, 0)
            block = o.at[rows(source), cols(far)]
            send(block, block, f1s.at[i, c], f1r.at[i, c, k], {"tp": far}).wait_recv()
            for p in range(1, size(1 - i)):
                send(block, block, f2s.at[i, p, c], f2r.at[i, p, c], {"tp": near(i, 0, p)}).start()

    for c in own:
        c.wait()
    for i, _, o in pairs:
        onward(0, i, o)

    def relay(k, _):
        source = lax.rem(me - k + n, n)
        for i, s, o in pairs:
            block = o.at[rows(source), cols(j)]
            send(block, block, s1s.at[i], s1r.at[i, k], {"sp": source}).wait_recv()
            onward(k, i, o)
        for i, s, o in pairs:
            relayed(k - 1, i, o)
        return 0

    lax.fori_loop(1, n, relay, 0)
    for i, _, o in pairs:
        relayed(n - 1, i, o)

    def take_carry(k, _):
        source = lax.rem(me - k + n, n)
        send(carry.at[source], carry.at[source], cs.at[k], cr.at[k], {"sp": source}).wait_recv()
        carried(k).wait_send()
        return 0

    lax.fori_loop(1, n, take_carry, 0)
    state = jnp.zeros((1, width), jnp.float32)
    for s in range(n):
        state = jnp.where(s < me, carry[s, 0:1] * state + carry[s, 1:2], state)
    whole = loc[...] + cum[...] * state
    hidden[...] = whole.astype(hidden.dtype)
    place = lax.broadcasted_iota(jnp.int32, whole.shape, 0)
    prev[...] = jnp.where(place >= 1, pltpu.roll(whole, 1, 0), state)
    for i, s, o in pairs:
        part = s.at[pl.ds(0, (n - 1) * cap)]
        send(part, part, s1s.at[i], s1r.at[i, 0], {"sp": lax.rem(me + 1, n)}).wait_send()
        mine = o.at[:, cols(j)]
        for p in range(1, size(i)):
            send(mine, mine, f1s.at[i, p], f1r.at[i, p, 0], {"tp": near(i, p, 0)}).wait_send()
        for p in range(1, size(1 - i)):
            for c in range(size(i)):
                sent = o.at[:, cols(near(i, size(i) - c, 0))]
                came = o.at[:, cols(near(i, size(i) - c, size(1 - i) - p))]
                to = {"tp": near(i, 0, p)}
                send(sent, sent, f2s.at[i, p, c], f2r.at[i, p, c], to).wait_send()
                send(came, came, f2s.at[i, p, c], f2r.at[i, p, c], to).wait_recv()


def return_kernel(
    n, m, pr, pick, hid, cot, nrm, gain, irms, omat, keep, carry, total_out, gow,
    out, hid_all, stage, red, back, mix_t, got, cum, loc, enters,
    rs, rr, bs, br, gs, gr, hs, hr, ms, mr, cs, cr, lsem,
):
    me, j = lax.axis_index("sp"), lax.axis_index("tp")
    tok = hid.shape[0]
    cap, q = pr.shape[0] // n, pr.shape[1] // m
    rows = lambda s: pl.ds(pl.multiple_of(s * cap, cap), cap)
    cols = lambda t: pl.ds(pl.multiple_of(t * q, q), q)
    greet(n, m, me, j)
    own = pltpu.make_async_copy(hid, hid_all.at[me], lsem)
    own.start()

    def spread(k, _):
        to = lax.rem(me + k, n)
        for p in range(1, m):
            far = lax.rem(j + p, m)
            send(
                pr.at[rows(to), cols(far)],
                stage.at[p - 1, rows(to)],
                rs.at[k],
                rr.at[k],
                {"tp": far},
            ).start()
        return 0

    lax.fori_loop(1, n + 1, spread, 0)

    def share(k, _):
        to = lax.rem(me + k, n)
        send(hid, hid_all.at[me], hs.at[k], hr.at[k], {"sp": to}).start()
        return 0

    lax.fori_loop(1, n, share, 0)

    def ship(k):
        to = lax.rem(me + k, n)
        return send(red.at[rows(to)], back.at[rows(me)], bs.at[k], br.at[k], {"sp": to})

    def reduce(k, _):
        to = lax.rem(me + k, n)
        block = stage.at[:, rows(to)]
        got = send(block, block, rs.at[k], rr.at[k], {"tp": lax.rem(j + 1, m)})
        got.wait_recv()
        got.wait_send()
        total = pr[rows(to), cols(j)].astype(jnp.float32)
        for p in range(1, m):
            total = total + stage[p - 1, rows(to)].astype(jnp.float32)
        red[rows(to)] = total.astype(red.dtype)

        @pl.when(k > 1)
        def _():
            ship(k - 1).start()

        return 0

    lax.fori_loop(1, n + 1, reduce, 0)
    back[rows(me)] = red[rows(me)]

    def collect(k, _):
        source = lax.rem(me - k + n, n)
        block = back.at[rows(source)]
        send(block, block, bs.at[k], br.at[k], {"sp": source}).wait_recv()
        return 0

    lax.fori_loop(1, n, collect, 0)
    total = jnp.dot(pick[...], back[...], preferred_element_type=jnp.float32)
    out[:, cols(j)] = total.astype(out.dtype)

    def finish(k, _):
        source = lax.rem(me - k + n, n)
        ship(k).wait_send()
        got = send(hid, hid_all.at[source], hs.at[k], hr.at[k], {"sp": source})
        got.wait_recv()
        got.wait_send()
        return 0

    lax.fori_loop(1, n, finish, 0)
    own.wait()
    mine = out.at[:, cols(j)]
    for p in range(1, m):
        send(mine, mine, gs.at[p], gr.at[p], {"tp": lax.rem(j + p, m)}).start()
    for p in range(1, m):
        far = lax.rem(j - p + m, m)
        theirs = out.at[:, cols(far)]
        send(mine, mine, gs.at[p], gr.at[p], {"tp": far}).wait_send()
        send(theirs, theirs, gs.at[p], gr.at[p], {"tp": far}).wait_recv()

    slab = mix_t.shape[0] // n
    width = keep.shape[1]
    slabs = lambda s: pl.ds(pl.multiple_of(s * slab, slab), slab)
    scale = gain[...]
    nhat = nrm[...].astype(jnp.float32) / scale
    gained = scale * out[...].astype(jnp.float32)
    stat = jnp.mean(gained * nhat, axis=1, keepdims=True)
    mixed = cot[...].astype(jnp.float32) + irms[...] * (gained - nhat * stat)
    mix_t[...] = mixed.T.astype(mix_t.dtype)
    loc[...] = jnp.dot(
        mixed.astype(omat.dtype), omat[...], preferred_element_type=jnp.float32
    )

    def blocks(k):
        to = lax.rem(me + k, n)
        return send(mix_t.at[slabs(to)], got.at[me], ms.at[k], mr.at[k], {"sp": to})

    def carried(k):
        to = lax.rem(me + k, n)
        return send(enters.at[me], enters.at[me], cs.at[k], cr.at[k], {"sp": to})

    def start_blocks(k, _):
        blocks(k).start()
        return 0

    lax.fori_loop(1, n, start_blocks, 0)
    place = lax.broadcasted_iota(jnp.int32, (tok, width), 0)
    here = keep[...]
    after = jnp.where(place < tok - 1, pltpu.roll(here, tok - 1, 0), 1.0)
    a, b = scan_rows(after, loc[...], True)
    enters[me] = jnp.broadcast_to(here[0:1] * b[0:1], (8, width))
    cum[...] = a
    loc[...] = b
    gow[...] = jnp.dot(mix_t[slabs(me)], hid_all[me], preferred_element_type=jnp.float32)

    def start(k, _):
        carried(k).start()
        return 0

    lax.fori_loop(1, n, start, 0)

    def add(k, _):
        source = lax.rem(me - k + n, n)
        send(got.at[source], got.at[source], ms.at[k], mr.at[k], {"sp": source}).wait_recv()
        blocks(k).wait_send()
        gow[...] += jnp.dot(got[source], hid_all[source], preferred_element_type=jnp.float32)
        return 0

    lax.fori_loop(1, n, add, 0)

    def take(k, _):
        source = lax.rem(me - k + n, n)
        send(enters.at[source], enters.at[source], cs.at[k], cr.at[k], {"sp": source}).wait_recv()
        carried(k).wait_send()
        return 0

    lax.fori_loop(1, n, take, 0)
    enter = jnp.zeros((1, width), jnp.float32)
    for s in range(n - 1, -1, -1):
        enter = jnp.where(s > me, carry[s, 0:1] * enter + enters[s, 0:1], enter)
    total_out[...] = loc[...] + cum[...] * enter


def call(kernel, n, m, outs, scratch, ident, *args):
    return pl.pallas_call(
        functools.partial(kernel, n, m),
        out_shape=tuple(jax.ShapeDtypeStruct(s, d) for s, d in outs),
        in_specs=[pl.BlockSpec(memory_space=pltpu.VMEM)] * len(args),
        out_specs=tuple(pl.BlockSpec(memory_space=pltpu.VMEM) for _ in outs),
        scratch_shapes=scratch,
        compiler_params=pltpu.CompilerParams(
            collective_id=ident, has_side_effects=True, vmem_limit_bytes=VMEM_LIMIT
        ),
    )(*args)


def shards(
    cotangent,
    normed,
    inverse_root_mean_square,
    expert_norm_scale,
    routes,
    route_probability_weight,
    gate_weight,
    up_weight,
    down_weight,
    recurrence_input,
    recurrence_gate_logits,
    input_gate_logits,
    channel_decay_weight,
    extra_log_decay,
    output_matrix,
):
    tok_rows, features = normed.shape
    n, m = lax.axis_size("sp"), lax.axis_size("tp")
    picks = routes.shape[1]
    capacity = 2 * picks * tok_rows // n
    slots = n * capacity
    q = features // m
    wide = max(sides(m))
    channels = recurrence_input.shape[1]
    f32, bf16 = jnp.float32, jnp.bfloat16
    dma = pltpu.SemaphoreType.DMA
    rowdims = (((0,), (0,)), ((), ()))
    coldims = (((1,), (1,)), ((), ()))

    chosen = routes.reshape(-1)
    member = chosen[:, None] == jnp.arange(n, dtype=jnp.int32)[None, :]
    order = jnp.arange(chosen.shape[0])
    below = (order[:, None] > order[None, :]).astype(bf16)
    before = jnp.dot(below, member.astype(bf16), preferred_element_type=f32)
    ranking = jnp.sum(jnp.where(member, before, 0.0), axis=1).astype(jnp.int32)
    landing = (chosen * capacity + ranking).reshape(tok_rows, picks)
    slot = jnp.arange(slots, dtype=jnp.int32)
    hits = [slot[:, None] == landing[:, k][None, :] for k in range(picks)]
    place = functools.reduce(jnp.logical_or, hits).astype(bf16)
    pick = functools.reduce(
        jnp.logical_or, [landing[:, k][:, None] == slot[None, :] for k in range(picks)]
    ).astype(bf16)
    share = sum(
        jnp.sum(jnp.where(h, route_probability_weight[:, k][None, :], 0.0), axis=1)
        for k, h in enumerate(hits)
    )
    offset = lax.axis_index("tp") * q
    normed_part = lax.dynamic_slice_in_dim(normed, offset, q, 1)
    cot_part = lax.dynamic_slice_in_dim(cotangent, offset, q, 1)
    token_send = jnp.dot(place, normed_part, preferred_element_type=f32).astype(bf16)
    grad_send = (
        share[:, None] * jnp.dot(place, cot_part, preferred_element_type=f32)
    ).astype(bf16)

    retention_factor = jax.nn.sigmoid(recurrence_gate_logits.astype(f32))
    admit = jax.nn.sigmoid(input_gate_logits.astype(f32))
    signal = recurrence_input.astype(f32)
    decay_speed = jax.nn.softplus(-channel_decay_weight)
    log_retention = -8.0 * retention_factor * decay_speed[None, :] + extra_log_decay
    keep = jnp.exp(log_retention)
    scale_in = jnp.sqrt(-jnp.expm1(2.0 * log_retention))
    driven = scale_in * admit * signal

    token_recv, grad_recv, hidden, state_prev, carry = call(
        dispatch_kernel, n, m,
        [
            ((slots, features), bf16),
            ((slots, features), bf16),
            ((tok_rows, channels), bf16),
            ((tok_rows, channels), f32),
            ((n, 8, channels), f32),
        ],
        [
            pltpu.VMEM((tok_rows, channels), f32),
            pltpu.VMEM((tok_rows, channels), f32),
            dma((2,)),
            dma((2, n)),
            dma((2, wide)),
            dma((2, wide, n)),
            dma((2, wide, wide)),
            dma((2, wide, wide)),
            dma((n,)),
            dma((n,)),
            dma((2,)),
        ],
        0, token_send, grad_send, keep, driven,
    )

    gate_w = gate_weight[0]
    up_w = up_weight[0]
    down_w = down_weight[0]
    gate_pre = jnp.dot(token_recv, gate_w, preferred_element_type=f32)
    up_pre = jnp.dot(token_recv, up_w, preferred_element_type=f32)
    sigma = jax.nn.sigmoid(gate_pre)
    swish = gate_pre * sigma
    active = (swish * up_pre).astype(bf16)
    d_active = lax.dot_general(grad_recv, down_w, coldims, preferred_element_type=f32)
    d_gate = (d_active * up_pre * sigma * (1.0 + gate_pre * (1.0 - sigma))).astype(bf16)
    d_up = (d_active * swish).astype(bf16)
    grad_down = lax.dot_general(active, grad_recv, rowdims, preferred_element_type=f32).astype(bf16)
    grad_gate = lax.dot_general(token_recv, d_gate, rowdims, preferred_element_type=f32).astype(bf16)
    grad_up = lax.dot_general(token_recv, d_up, rowdims, preferred_element_type=f32).astype(bf16)
    partial_rows = lax.dot_general(d_gate, gate_w, coldims, preferred_element_type=f32)
    partial_rows = partial_rows + lax.dot_general(d_up, up_w, coldims, preferred_element_type=f32)

    total, grad_out_weight = call(
        return_kernel, n, m,
        [((tok_rows, channels), f32), ((features // n, channels), f32)],
        [
            pltpu.VMEM((tok_rows, features), bf16),
            pltpu.VMEM((n, tok_rows, channels), bf16),
            pltpu.VMEM((m - 1, slots, q), bf16),
            pltpu.VMEM((slots, q), bf16),
            pltpu.VMEM((slots, q), bf16),
            pltpu.VMEM((features, tok_rows), bf16),
            pltpu.VMEM((n, features // n, tok_rows), bf16),
            pltpu.VMEM((tok_rows, channels), f32),
            pltpu.VMEM((tok_rows, channels), f32),
            pltpu.VMEM((n, 8, channels), f32),
            dma((n + 1,)),
            dma((n + 1,)),
            dma((n,)),
            dma((n,)),
            dma((m,)),
            dma((m,)),
            dma((n,)),
            dma((n,)),
            dma((n,)),
            dma((n,)),
            dma((n,)),
            dma((n,)),
            dma,
        ],
        1,
        partial_rows.astype(bf16),
        pick,
        hidden,
        cotangent,
        normed,
        expert_norm_scale[None, :],
        inverse_root_mean_square[:, None],
        output_matrix,
        keep,
        carry,
    )
    grad_rec_input = total * scale_in * admit
    grad_input_gate = total * scale_in * signal * admit * (1.0 - admit)
    d_log = total * state_prev * keep - total * admit * signal * keep * keep / scale_in
    grad_decay_gate = (
        d_log * (-8.0 * decay_speed[None, :]) * retention_factor * (1.0 - retention_factor)
    )
    return (
        grad_gate[None],
        grad_up[None],
        grad_down[None],
        grad_out_weight,
        grad_rec_input,
        grad_decay_gate,
        grad_input_gate,
    )


def solution(mesh):
    return jax.shard_map(
        shards,
        mesh=mesh,
        in_specs=(
            P("sp", None),
            P("sp", None),
            P("sp"),
            P(),
            P("sp", None),
            P("sp", None),
            P("sp", None, "tp"),
            P("sp", None, "tp"),
            P("sp", "tp", None),
            P("sp", "tp"),
            P("sp", "tp"),
            P("sp", "tp"),
            P("tp"),
            P("sp", "tp"),
            P(None, "tp"),
        ),
        out_specs=(
            P("sp", None, "tp"),
            P("sp", None, "tp"),
            P("sp", "tp", None),
            P("sp", "tp"),
            P("sp", "tp"),
            P("sp", "tp"),
            P("sp", "tp"),
        ),
        check_vma=False,
    )
```

```python
import functools

import jax
import jax.numpy as jnp
from jax import lax
from jax.experimental import pallas as pl
from jax.experimental.pallas import tpu as pltpu
from jax.sharding import PartitionSpec as P

MESH = pl.DeviceIdType.MESH
VMEM_LIMIT = 56 * 1024 * 1024


def sides(m):
    high = max(d for d in range(1, m + 1) if m % d == 0 and d * d <= m)
    return high, m // high


def greet(n, m, me, j):
    barrier = pltpu.get_barrier_semaphore()
    for k in range(1, n):
        pl.semaphore_signal(
            barrier, inc=1, device_id={"sp": lax.rem(me + k, n)}, device_id_type=MESH
        )
    for p in range(1, m):
        pl.semaphore_signal(
            barrier, inc=1, device_id={"tp": lax.rem(j + p, m)}, device_id_type=MESH
        )
    pl.semaphore_wait(barrier, n - 1 + m - 1)


def send(src, dst, send_sem, recv_sem, where):
    return pltpu.make_async_remote_copy(
        src_ref=src,
        dst_ref=dst,
        send_sem=send_sem,
        recv_sem=recv_sem,
        device_id=where,
        device_id_type=MESH,
    )


def scan_rows(a, b, reverse):
    rows = a.shape[0]
    place = lax.broadcasted_iota(jnp.int32, a.shape, 0)
    step = 1
    while step < rows:
        if reverse:
            known = place < rows - step
            shift = rows - step
        else:
            known = place >= step
            shift = step
        a_far = jnp.where(known, pltpu.roll(a, shift, 0), 1.0)
        b_far = jnp.where(known, pltpu.roll(b, shift, 0), 0.0)
        b = a * b_far + b
        a = a * a_far
        step *= 2
    return a, b


def dispatch_kernel(
    n, m, xs, ys, keep, driven, xo, yo, hidden, prev, carry,
    cum, loc, s1s, s1r, f1s, f1r, f2s, f2r, cs, cr, lsem,
):
    me, j = lax.axis_index("sp"), lax.axis_index("tp")
    cap, q = xs.shape[0] // n, xs.shape[1]
    tok = keep.shape[0]
    rows = lambda s: pl.ds(pl.multiple_of(s * cap, cap), cap)
    cols = lambda t: pl.ds(pl.multiple_of(t * q, q), q)
    pairs = ((0, xs, xo), (1, ys, yo))
    high, low = sides(m)
    upper, lower = lax.div(j, low), lax.rem(j, low)

    def size(i):
        return low if i == 0 else high

    def near(i, along, across):
        up, down = (across, along) if i == 0 else (along, across)
        return lax.rem(upper + up, high) * low + lax.rem(lower + down, low)

    a, b = scan_rows(keep[...], driven[...], False)
    cum[...] = a
    loc[...] = b
    width = a.shape[1]
    carry[me] = jnp.concatenate(
        [a[tok - 1 : tok], b[tok - 1 : tok], jnp.zeros((6, width), jnp.float32)], axis=0
    )
    greet(n, m, me, j)

    def first(k):
        to = lax.rem(me + k, n)
        return [
            send(s.at[rows(to)], o.at[rows(me), cols(j)], s1s.at[i], s1r.at[i, k], {"sp": to})
            for i, s, o in pairs
        ]

    def carried(k):
        to = lax.rem(me + k, n)
        return send(carry.at[me], carry.at[me], cs.at[k], cr.at[k], {"sp": to})

    own = [
        pltpu.make_async_copy(s.at[rows(me)], o.at[rows(me), cols(j)], lsem.at[i])
        for i, s, o in pairs
    ]
    for c in own:
        c.start()

    def start_carry(k, _):
        carried(k).start()
        return 0

    lax.fori_loop(1, n, start_carry, 0)

    def start_first(k, _):
        for c in first(k):
            c.start()
        return 0

    lax.fori_loop(1, n, start_first, 0)

    def onward(k, i, o):
        source = lax.rem(me - k + n, n)
        block = o.at[rows(source), cols(j)]
        for p in range(1, size(i)):
            send(block, block, f1s.at[i, p], f1r.at[i, p, k], {"tp": near(i, p, 0)}).start()
        for p in range(1, size(1 - i)):
            send(block, block, f2s.at[i, p, 0], f2r.at[i, p, 0], {"tp": near(i, 0, p)}).start()

    def relayed(k, i, o):
        source = lax.rem(me - k + n, n)
        for c in range(1, size(i)):
            far = near(i, size(i) - c, 0)
            block = o.at[rows(source), cols(far)]
            send(block, block, f1s.at[i, c], f1r.at[i, c, k], {"tp": far}).wait_recv()
            for p in range(1, size(1 - i)):
                send(block, block, f2s.at[i, p, c], f2r.at[i, p, c], {"tp": near(i, 0, p)}).start()

    for c in own:
        c.wait()
    for i, _, o in pairs:
        onward(0, i, o)

    def relay(k, _):
        source = lax.rem(me - k + n, n)
        for i, s, o in pairs:
            block = o.at[rows(source), cols(j)]
            send(block, block, s1s.at[i], s1r.at[i, k], {"sp": source}).wait_recv()
            onward(k, i, o)
        for i, s, o in pairs:
            relayed(k - 1, i, o)
        return 0

    lax.fori_loop(1, n, relay, 0)
    for i, _, o in pairs:
        relayed(n - 1, i, o)

    def take_carry(k, _):
        source = lax.rem(me - k + n, n)
        send(carry.at[source], carry.at[source], cs.at[k], cr.at[k], {"sp": source}).wait_recv()
        carried(k).wait_send()
        return 0

    lax.fori_loop(1, n, take_carry, 0)
    state = jnp.zeros((1, width), jnp.float32)
    for s in range(n):
        state = jnp.where(s < me, carry[s, 0:1] * state + carry[s, 1:2], state)
    whole = loc[...] + cum[...] * state
    hidden[...] = whole.astype(hidden.dtype)
    place = lax.broadcasted_iota(jnp.int32, whole.shape, 0)
    prev[...] = jnp.where(place >= 1, pltpu.roll(whole, 1, 0), state)
    for i, s, o in pairs:
        part = s.at[pl.ds(0, (n - 1) * cap)]
        send(part, part, s1s.at[i], s1r.at[i, 0], {"sp": lax.rem(me + 1, n)}).wait_send()
        mine = o.at[:, cols(j)]
        for p in range(1, size(i)):
            send(mine, mine, f1s.at[i, p], f1r.at[i, p, 0], {"tp": near(i, p, 0)}).wait_send()
        for p in range(1, size(1 - i)):
            for c in range(size(i)):
                sent = o.at[:, cols(near(i, size(i) - c, 0))]
                came = o.at[:, cols(near(i, size(i) - c, size(1 - i) - p))]
                to = {"tp": near(i, 0, p)}
                send(sent, sent, f2s.at[i, p, c], f2r.at[i, p, c], to).wait_send()
                send(came, came, f2s.at[i, p, c], f2r.at[i, p, c], to).wait_recv()


def return_kernel(
    n, m, pr, pick, hid, cot, nrm, gain, irms, omat, keep, carry, total_out, gow,
    out, hid_all, stage, red, back, mix_t, got, cum, loc, enters,
    rs, rr, bs, br, gs, gr, hs, hr, ms, mr, cs, cr, lsem,
):
    me, j = lax.axis_index("sp"), lax.axis_index("tp")
    tok = hid.shape[0]
    cap, q = pr.shape[0] // n, pr.shape[1] // m
    rows = lambda s: pl.ds(pl.multiple_of(s * cap, cap), cap)
    cols = lambda t: pl.ds(pl.multiple_of(t * q, q), q)
    greet(n, m, me, j)
    own = pltpu.make_async_copy(hid, hid_all.at[me], lsem)
    own.start()

    def spread(k, _):
        to = lax.rem(me + k, n)
        for p in range(1, m):
            far = lax.rem(j + p, m)
            send(
                pr.at[rows(to), cols(far)],
                stage.at[p - 1, rows(to)],
                rs.at[k],
                rr.at[k],
                {"tp": far},
            ).start()
        return 0

    lax.fori_loop(1, n + 1, spread, 0)

    def share(k, _):
        to = lax.rem(me + k, n)
        send(hid, hid_all.at[me], hs.at[k], hr.at[k], {"sp": to}).start()
        return 0

    lax.fori_loop(1, n, share, 0)

    def ship(k):
        to = lax.rem(me + k, n)
        return send(red.at[rows(to)], back.at[rows(me)], bs.at[k], br.at[k], {"sp": to})

    def reduce(k, _):
        to = lax.rem(me + k, n)
        block = stage.at[:, rows(to)]
        got = send(block, block, rs.at[k], rr.at[k], {"tp": lax.rem(j + 1, m)})
        got.wait_recv()
        got.wait_send()
        total = pr[rows(to), cols(j)].astype(jnp.float32)
        for p in range(1, m):
            total = total + stage[p - 1, rows(to)].astype(jnp.float32)
        red[rows(to)] = total.astype(red.dtype)

        @pl.when(k > 1)
        def _():
            ship(k - 1).start()

        return 0

    lax.fori_loop(1, n + 1, reduce, 0)
    back[rows(me)] = red[rows(me)]

    def collect(k, _):
        source = lax.rem(me - k + n, n)
        block = back.at[rows(source)]
        send(block, block, bs.at[k], br.at[k], {"sp": source}).wait_recv()
        return 0

    lax.fori_loop(1, n, collect, 0)
    total = jnp.dot(pick[...], back[...], preferred_element_type=jnp.float32)
    out[:, cols(j)] = total.astype(out.dtype)

    def finish(k, _):
        source = lax.rem(me - k + n, n)
        ship(k).wait_send()
        got = send(hid, hid_all.at[source], hs.at[k], hr.at[k], {"sp": source})
        got.wait_recv()
        got.wait_send()
        return 0

    lax.fori_loop(1, n, finish, 0)
    own.wait()
    mine = out.at[:, cols(j)]
    for p in range(1, m):
        send(mine, mine, gs.at[p], gr.at[p], {"tp": lax.rem(j + p, m)}).start()
    for p in range(1, m):
        far = lax.rem(j - p + m, m)
        theirs = out.at[:, cols(far)]
        send(mine, mine, gs.at[p], gr.at[p], {"tp": far}).wait_send()
        send(theirs, theirs, gs.at[p], gr.at[p], {"tp": far}).wait_recv()

    slab = mix_t.shape[0] // n
    width = keep.shape[1]
    slabs = lambda s: pl.ds(pl.multiple_of(s * slab, slab), slab)
    scale = gain[...]
    nhat = nrm[...].astype(jnp.float32) / scale
    gained = scale * out[...].astype(jnp.float32)
    stat = jnp.mean(gained * nhat, axis=1, keepdims=True)
    mixed = cot[...].astype(jnp.float32) + irms[...] * (gained - nhat * stat)
    mix_t[...] = mixed.T.astype(mix_t.dtype)
    loc[...] = jnp.dot(
        mixed.astype(omat.dtype), omat[...], preferred_element_type=jnp.float32
    )

    def blocks(k):
        to = lax.rem(me + k, n)
        return send(mix_t.at[slabs(to)], got.at[me], ms.at[k], mr.at[k], {"sp": to})

    def carried(k):
        to = lax.rem(me + k, n)
        return send(enters.at[me], enters.at[me], cs.at[k], cr.at[k], {"sp": to})

    def start_blocks(k, _):
        blocks(k).start()
        return 0

    lax.fori_loop(1, n, start_blocks, 0)
    place = lax.broadcasted_iota(jnp.int32, (tok, width), 0)
    here = keep[...]
    after = jnp.where(place < tok - 1, pltpu.roll(here, tok - 1, 0), 1.0)
    a, b = scan_rows(after, loc[...], True)
    enters[me] = jnp.broadcast_to(here[0:1] * b[0:1], (8, width))
    cum[...] = a
    loc[...] = b
    gow[...] = jnp.dot(mix_t[slabs(me)], hid_all[me], preferred_element_type=jnp.float32)

    def start(k, _):
        carried(k).start()
        return 0

    lax.fori_loop(1, n, start, 0)

    def add(k, _):
        source = lax.rem(me - k + n, n)
        send(got.at[source], got.at[source], ms.at[k], mr.at[k], {"sp": source}).wait_recv()
        blocks(k).wait_send()
        gow[...] += jnp.dot(got[source], hid_all[source], preferred_element_type=jnp.float32)
        return 0

    lax.fori_loop(1, n, add, 0)

    def take(k, _):
        source = lax.rem(me - k + n, n)
        send(enters.at[source], enters.at[source], cs.at[k], cr.at[k], {"sp": source}).wait_recv()
        carried(k).wait_send()
        return 0

    lax.fori_loop(1, n, take, 0)
    enter = jnp.zeros((1, width), jnp.float32)
    for s in range(n - 1, -1, -1):
        enter = jnp.where(s > me, carry[s, 0:1] * enter + enters[s, 0:1], enter)
    total_out[...] = loc[...] + cum[...] * enter


def call(kernel, n, m, outs, scratch, ident, *args, loose=0):
    return pl.pallas_call(
        functools.partial(kernel, n, m),
        out_shape=tuple(jax.ShapeDtypeStruct(s, d) for s, d in outs),
        in_specs=[pl.BlockSpec(memory_space=pltpu.VMEM)] * len(args),
        out_specs=tuple(
            pl.BlockSpec(memory_space=pl.ANY if at < loose else pltpu.VMEM)
            for at in range(len(outs))
        ),
        scratch_shapes=scratch,
        compiler_params=pltpu.CompilerParams(
            collective_id=ident, has_side_effects=True, vmem_limit_bytes=VMEM_LIMIT
        ),
    )(*args)


def shards(
    cotangent,
    normed,
    inverse_root_mean_square,
    expert_norm_scale,
    routes,
    route_probability_weight,
    gate_weight,
    up_weight,
    down_weight,
    recurrence_input,
    recurrence_gate_logits,
    input_gate_logits,
    channel_decay_weight,
    extra_log_decay,
    output_matrix,
):
    tok_rows, features = normed.shape
    n, m = lax.axis_size("sp"), lax.axis_size("tp")
    picks = routes.shape[1]
    capacity = 2 * picks * tok_rows // n
    slots = n * capacity
    q = features // m
    wide = max(sides(m))
    channels = recurrence_input.shape[1]
    f32, bf16 = jnp.float32, jnp.bfloat16
    dma = pltpu.SemaphoreType.DMA
    rowdims = (((0,), (0,)), ((), ()))
    coldims = (((1,), (1,)), ((), ()))

    chosen = routes.reshape(-1)
    member = chosen[:, None] == jnp.arange(n, dtype=jnp.int32)[None, :]
    order = jnp.arange(chosen.shape[0])
    below = (order[:, None] > order[None, :]).astype(bf16)
    before = jnp.dot(below, member.astype(bf16), preferred_element_type=f32)
    ranking = jnp.sum(jnp.where(member, before, 0.0), axis=1).astype(jnp.int32)
    landing = (chosen * capacity + ranking).reshape(tok_rows, picks)
    slot = jnp.arange(slots, dtype=jnp.int32)
    hits = [slot[:, None] == landing[:, k][None, :] for k in range(picks)]
    place = functools.reduce(jnp.logical_or, hits).astype(bf16)
    pick = functools.reduce(
        jnp.logical_or, [landing[:, k][:, None] == slot[None, :] for k in range(picks)]
    ).astype(bf16)
    share = sum(
        jnp.sum(jnp.where(h, route_probability_weight[:, k][None, :], 0.0), axis=1)
        for k, h in enumerate(hits)
    )
    offset = lax.axis_index("tp") * q
    normed_part = lax.dynamic_slice_in_dim(normed, offset, q, 1)
    cot_part = lax.dynamic_slice_in_dim(cotangent, offset, q, 1)
    token_send = jnp.dot(place, normed_part, preferred_element_type=f32).astype(bf16)
    grad_send = (
        share[:, None] * jnp.dot(place, cot_part, preferred_element_type=f32)
    ).astype(bf16)

    retention_factor = jax.nn.sigmoid(recurrence_gate_logits.astype(f32))
    admit = jax.nn.sigmoid(input_gate_logits.astype(f32))
    signal = recurrence_input.astype(f32)
    decay_speed = jax.nn.softplus(-channel_decay_weight)
    log_retention = -8.0 * retention_factor * decay_speed[None, :] + extra_log_decay
    keep = jnp.exp(log_retention)
    scale_in = jnp.sqrt(-jnp.expm1(2.0 * log_retention))
    driven = scale_in * admit * signal

    token_recv, grad_recv, hidden, state_prev, carry = call(
        dispatch_kernel, n, m,
        [
            ((slots, features), bf16),
            ((slots, features), bf16),
            ((tok_rows, channels), bf16),
            ((tok_rows, channels), f32),
            ((n, 8, channels), f32),
        ],
        [
            pltpu.VMEM((tok_rows, channels), f32),
            pltpu.VMEM((tok_rows, channels), f32),
            dma((2,)),
            dma((2, n)),
            dma((2, wide)),
            dma((2, wide, n)),
            dma((2, wide, wide)),
            dma((2, wide, wide)),
            dma((n,)),
            dma((n,)),
            dma((2,)),
        ],
        0, token_send, grad_send, keep, driven, loose=2,
    )

    gate_w = gate_weight[0]
    up_w = up_weight[0]
    down_w = down_weight[0]
    gate_pre = jnp.dot(token_recv, gate_w, preferred_element_type=f32)
    up_pre = jnp.dot(token_recv, up_w, preferred_element_type=f32)
    sigma = jax.nn.sigmoid(gate_pre)
    swish = gate_pre * sigma
    active = (swish * up_pre).astype(bf16)
    d_active = lax.dot_general(grad_recv, down_w, coldims, preferred_element_type=f32)
    d_gate = (d_active * up_pre * sigma * (1.0 + gate_pre * (1.0 - sigma))).astype(bf16)
    d_up = (d_active * swish).astype(bf16)
    grad_down = lax.dot_general(active, grad_recv, rowdims, preferred_element_type=f32).astype(bf16)
    grad_gate = lax.dot_general(token_recv, d_gate, rowdims, preferred_element_type=f32).astype(bf16)
    grad_up = lax.dot_general(token_recv, d_up, rowdims, preferred_element_type=f32).astype(bf16)
    partial_rows = lax.dot_general(d_gate, gate_w, coldims, preferred_element_type=f32)
    partial_rows = partial_rows + lax.dot_general(d_up, up_w, coldims, preferred_element_type=f32)

    total, grad_out_weight = call(
        return_kernel, n, m,
        [((tok_rows, channels), f32), ((features // n, channels), f32)],
        [
            pltpu.VMEM((tok_rows, features), bf16),
            pltpu.VMEM((n, tok_rows, channels), bf16),
            pltpu.VMEM((m - 1, slots, q), bf16),
            pltpu.VMEM((slots, q), bf16),
            pltpu.VMEM((slots, q), bf16),
            pltpu.VMEM((features, tok_rows), bf16),
            pltpu.VMEM((n, features // n, tok_rows), bf16),
            pltpu.VMEM((tok_rows, channels), f32),
            pltpu.VMEM((tok_rows, channels), f32),
            pltpu.VMEM((n, 8, channels), f32),
            dma((n + 1,)),
            dma((n + 1,)),
            dma((n,)),
            dma((n,)),
            dma((m,)),
            dma((m,)),
            dma((n,)),
            dma((n,)),
            dma((n,)),
            dma((n,)),
            dma((n,)),
            dma((n,)),
            dma,
        ],
        1,
        partial_rows.astype(bf16),
        pick,
        hidden,
        cotangent,
        normed,
        expert_norm_scale[None, :],
        inverse_root_mean_square[:, None],
        output_matrix,
        keep,
        carry,
    )
    grad_rec_input = total * scale_in * admit
    grad_input_gate = total * scale_in * signal * admit * (1.0 - admit)
    d_log = total * state_prev * keep - total * admit * signal * keep * keep / scale_in
    grad_decay_gate = (
        d_log * (-8.0 * decay_speed[None, :]) * retention_factor * (1.0 - retention_factor)
    )
    return (
        grad_gate[None],
        grad_up[None],
        grad_down[None],
        grad_out_weight,
        grad_rec_input,
        grad_decay_gate,
        grad_input_gate,
    )


def solution(mesh):
    return jax.shard_map(
        shards,
        mesh=mesh,
        in_specs=(
            P("sp", None),
            P("sp", None),
            P("sp"),
            P(),
            P("sp", None),
            P("sp", None),
            P("sp", None, "tp"),
            P("sp", None, "tp"),
            P("sp", "tp", None),
            P("sp", "tp"),
            P("sp", "tp"),
            P("sp", "tp"),
            P("tp"),
            P("sp", "tp"),
            P(None, "tp"),
        ),
        out_specs=(
            P("sp", None, "tp"),
            P("sp", None, "tp"),
            P("sp", "tp", None),
            P("sp", "tp"),
            P("sp", "tp"),
            P("sp", "tp"),
            P("sp", "tp"),
        ),
        check_vma=False,
    )
```
